32 devices in a mesh: grp: 2 (over x), ep: 16 (over z, y, core).
Axes of the slice: x: 2, y: 2, z: 4, core: 2. Of those that a mesh axis runs over, the one named last changes fastest.
Arguments:
- tokens: bfloat16 [8192, 2048], P(('grp', 'ep')), parts along dimension 0, may hold values from -6 to 6
- norm_gain: float32 [2048], replicated, may hold values from 0.1 to 1.9
- route_ids: int32 [8192, 2], P(('grp', 'ep')), parts along dimension 0, may hold values from 0 to 15, as said below
- route_slots: int32 [8192, 2], P(('grp', 'ep')), parts along dimension 0, may hold values from 0 to 47, as said below
- route_weights: float32 [8192, 2], P(('grp', 'ep')), parts along dimension 0, may hold values from 0.1 to 1
- w_gate: bfloat16 [16, 2048, 512], P('ep'), may hold values from -0.125 to 0.125
- w_up: bfloat16 [16, 2048, 512], P('ep'), may hold values from -0.125 to 0.125
- w_down: bfloat16 [16, 512, 2048], P('ep'), may hold values from -0.25 to 0.25
Outputs:
- expert_mix: bfloat16 [8192, 2048], P(('grp', 'ep')), parts along dimension 0
The draws below stay inside these ranges and needn't reach their ends.
There are 2 independent parts, one for each index of `grp`. The reference program is written for one: setup_inputs(seed, part) draws one part's arguments, and reference() takes and returns one part's arrays. A program takes and returns all parts, laid end to end along the dimension named above; an argument that names none is the same for every part. Nothing has to cross between parts.
Inputs may be any that keep to these rules, and one draw needn't show every extreme that they name: `route_ids`: expert e belongs to group e // 4. Each token names 2 different experts of one group. In each aligned block of 256 tokens (the rows of one device) no expert is named more than 48 times, and some expert exactly 48 times. `route_slots`: in each aligned block of 256 tokens, the entries that name one expert hold distinct slots 0, 1, ... up to their count less one.
All inputs are finite; a program needn't handle non-finite values.
Results may differ from the reference program's by a relative error of at most 0.007.
Values may be sent and summed in bfloat16 or wider, within the bound.
A program may use at most 64 MiB of HBM per device.

```python
import math
import jax
import jax.numpy as jnp
from jax import lax

D = 2048
FE = 512
TOPK = 2
TOK_DEV = 256
EXPERTS = 16
CAP = 48
TOKENS = 4096


def route_table(key):
    n_blocks = TOKENS // TOK_DEV
    per_group = EXPERTS // 4
    busy_count = CAP * per_group // 2
    rest_count = TOK_DEV - busy_count
    block_keys = jax.random.split(jax.random.fold_in(key, 7), n_blocks)

    def one_block(block_key):
        key_busy, key_first, key_second, key_perm, key_base, key_shift = jax.random.split(block_key, 6)
        busy = jax.random.randint(key_busy, (), 0, 4)
        low_first = jnp.maximum(0, rest_count - 2 * busy_count)
        high_first = jnp.minimum(busy_count, rest_count)
        count_first = jax.random.randint(key_first, (), low_first, high_first + 1)
        low_second = jnp.maximum(0, rest_count - count_first - busy_count)
        high_second = jnp.minimum(busy_count, rest_count - count_first)
        count_second = jax.random.randint(key_second, (), low_second, high_second + 1)
        others = jnp.stack([count_first, count_second, rest_count - count_first - count_second]).astype(jnp.int32)
        group_ids = jnp.arange(4, dtype=jnp.int32)
        other_idx = jnp.clip(group_ids - (group_ids > busy).astype(jnp.int32), 0, 2)
        counts = jnp.where(group_ids == busy, busy_count, others[other_idx]).astype(jnp.int32)
        ends = jnp.cumsum(counts)
        starts = ends - counts
        places = jnp.arange(TOK_DEV, dtype=jnp.int32)
        group_sorted = jnp.sum((places[:, None] >= ends[None, :3]).astype(jnp.int32), axis=1)
        rank_sorted = places - starts[group_sorted]
        perm = jax.random.permutation(key_perm, TOK_DEV)
        group_tok = jnp.zeros((TOK_DEV,), jnp.int32).at[perm].set(group_sorted)
        rank_tok = jnp.zeros((TOK_DEV,), jnp.int32).at[perm].set(rank_sorted)
        base = jax.random.randint(key_base, (4,), 0, per_group)
        shift = jax.random.randint(key_shift, (4,), 1, per_group)
        first = group_tok * per_group + (base[group_tok] + rank_tok) % per_group
        second = group_tok * per_group + (base[group_tok] + rank_tok + shift[group_tok]) % per_group
        ids = jnp.stack([first, second], axis=1).astype(jnp.int32)
        flat_ids = ids.reshape(-1)
        onehot = (flat_ids[:, None] == jnp.arange(EXPERTS, dtype=jnp.int32)[None, :]).astype(jnp.int32)
        slots = jnp.sum(jnp.cumsum(onehot, axis=0) * onehot, axis=1) - 1
        return (ids, slots.reshape(TOK_DEV, 2).astype(jnp.int32))
    ids, slots = jax.vmap(one_block)(block_keys)
    return (ids.reshape(TOKENS, 2), slots.reshape(TOKENS, 2))


def draw_route_ids(key, part):
    return route_table(key)[0]


def draw_route_slots(key, part):
    return route_table(key)[1]


def block_levels(rng, extent, shards, low, largest):
    loudness, own = 1.0, jax.random.fold_in(rng, 6)
    for dim, shards_of in shards:
        heights = jnp.exp(jax.random.uniform(jax.random.fold_in(own, dim), (shards_of,), jnp.float32, low / len(shards), largest / len(shards)))
        loudness = loudness * jnp.repeat(heights, extent[dim] // shards_of).reshape([-1 if axis == dim else 1 for axis in range(len(extent))])
    return loudness


def scatter_about(key, dims, spread, reach, cuts=(), kind=jnp.bfloat16):
    drawn = spread * jax.random.normal(key, dims, jnp.float32)
    if cuts:
        drawn = drawn * block_levels(key, dims, cuts, -0.22, 0.18)
    return jnp.clip(drawn, -reach, reach).astype(kind)


def setup_inputs(seed: int = 0, part: int = 0) -> dict:
    streams_of = jax.random.split(jax.random.key(seed), 9)
    own_keys = jax.random.split(jax.random.fold_in(streams_of[8], part), 9)
    return {
        "tokens": scatter_about(own_keys[0], (TOKENS, D), 1.0, 6.0, ((0, 16),)),
        "norm_gain": jnp.clip(1.0 + 0.18 * jax.random.normal(streams_of[1], (D,), jnp.float32), 0.1, 1.9),
        "route_ids": draw_route_ids(jax.random.fold_in(jax.random.fold_in(streams_of[8], part), 71), part),
        "route_slots": draw_route_slots(jax.random.fold_in(jax.random.fold_in(streams_of[8], part), 71), part),
        "route_weights": jnp.clip(jnp.exp(math.log(1.0) - 2.3025851 * jax.random.uniform(own_keys[4], (TOKENS, TOPK), jnp.float32) ** block_levels(own_keys[4], (TOKENS, TOPK), ((0, 16),), -0.2, 0.2)), 0.1, 1.0),
        "w_gate": scatter_about(streams_of[5], (EXPERTS, D, FE), D ** -0.5, 0.125, ((0, 16),)),
        "w_up": scatter_about(streams_of[6], (EXPERTS, D, FE), D ** -0.5, 0.125, ((0, 16),)),
        "w_down": scatter_about(streams_of[7], (EXPERTS, FE, D), FE ** -0.5, 0.25, ((0, 16),)),
    }


def reference(tokens, norm_gain, route_ids, route_slots, route_weights, w_gate, w_up, w_down):
    tok_f32 = tokens.astype(jnp.float32)
    scale = lax.rsqrt(lax.optimization_barrier(jnp.mean(tok_f32 * tok_f32, axis=-1, keepdims=True)) + 1e-06)
    normed = (tok_f32 * scale * norm_gain.astype(jnp.float32)).astype(jnp.bfloat16)
    n_blocks = TOKENS // TOK_DEV
    block_of = (jnp.arange(TOKENS, dtype=jnp.int32) // TOK_DEV).astype(jnp.int32)
    place_idx = (route_ids * (n_blocks * CAP) + block_of[:, None] * CAP + route_slots).astype(jnp.int32)
    buffer = jnp.zeros((EXPERTS * n_blocks * CAP, D), jnp.bfloat16)
    buffer = buffer.at[place_idx.reshape(-1)].set(jnp.repeat(normed, TOPK, axis=0))
    buffer = buffer.reshape(EXPERTS, n_blocks * CAP, D)

    def expert_apply(args):
        rows_in, gate_w, up_w, down_w = args
        gate_act = jnp.dot(rows_in, gate_w, preferred_element_type=jnp.float32)
        up_act = jnp.dot(rows_in, up_w, preferred_element_type=jnp.float32)
        hidden = (jax.nn.silu(gate_act) * up_act).astype(jnp.bfloat16)
        return jnp.dot(hidden, down_w, preferred_element_type=jnp.float32).astype(jnp.bfloat16)
    results = lax.map(expert_apply, (buffer, w_gate, w_up, w_down))
    flat_rows = results.reshape(EXPERTS * n_blocks * CAP, D)
    picked = flat_rows[place_idx].astype(jnp.float32)
    mixed = lax.optimization_barrier(jnp.sum(route_weights[:, :, None] * picked, axis=1))
    return mixed.astype(jnp.bfloat16)
```

```python
import functools

import jax
import jax.numpy as jnp
from jax import lax
from jax.experimental import pallas as pl
from jax.experimental.pallas import tpu as pltpu
from jax.sharding import PartitionSpec as P

GROUPS = 4
META = 128
ORDER = (2, 1, 3)
NT = (((1,), (1,)), ((), ()))
F32 = jnp.float32
BF16 = jnp.bfloat16


def flip(index, bits):
    out, weight = index, 1
    while weight <= bits:
        if bits & weight:
            out = out + weight * (1 - 2 * ((index // weight) % 2))
        weight *= 2
    return out


def kernel(
    peers, cap, capp,
    tok, gain, ids, slots, wts, wg_hbm, wu_hbm, wd_hbm,
    out,
    normed, x_out, x_in, y_out, e_in, hid, r_out, r_in, m_out, h_in, wg, wu, wd,
    w_sem, xs, xr, ys, yr, rs, rr, hs, hr,
):
    rows, feat = tok.shape
    ffn = wg.shape[1]
    block = x_out.shape[1]
    spread = peers * capp
    me = lax.axis_index("ep")
    group, rank = me // peers, me % peers
    shift = peers.bit_length() - 1

    def at(d, j):
        return {"ep": flip(group, d) * peers + flip(rank, j)}

    barrier = pltpu.get_barrier_semaphore()
    for d in range(1, GROUPS):
        pl.semaphore_signal(barrier, inc=1, device_id=at(d, 0), device_id_type=pl.DeviceIdType.MESH)
    for j in range(1, peers):
        pl.semaphore_signal(barrier, inc=1, device_id=at(0, j), device_id_type=pl.DeviceIdType.MESH)

    loads = [
        pltpu.make_async_copy(src, dst, w_sem.at[i])
        for i, (src, dst) in enumerate(((wg_hbm, wg), (wu_hbm, wu), (wd_hbm, wd)))
    ]
    for load in loads:
        load.start()

    def remote(src, dst, send, recv, where):
        return pltpu.make_async_remote_copy(
            src_ref=src, dst_ref=dst, send_sem=send, recv_sem=recv,
            device_id=where, device_id_type=pl.DeviceIdType.MESH,
        )

    step = 32

    def norm_rows(i, carry):
        at_rows = pl.ds(i * step, step)
        v = tok[at_rows, :].astype(F32)
        scale = lax.rsqrt(jnp.mean(v * v, axis=-1, keepdims=True) + 1e-06)
        normed[at_rows, :feat] = (v * scale * gain[...]).astype(BF16)
        return carry

    lax.fori_loop(0, rows // step, norm_rows, 0)

    lane = lax.broadcasted_iota(jnp.int32, (rows, META), 1)
    meta = jnp.zeros((rows, META), F32)
    for k in range(2):
        e = ids[:, k:k + 1]
        code = (((e & (peers - 1)) ^ rank) * capp + slots[:, k:k + 1] + 1).astype(F32)
        meta = jnp.where(lane == k, code, meta)
        w = wts[:, k:k + 1]
        for part in range(3):
            piece = w.astype(BF16).astype(F32)
            meta = jnp.where(lane == 2 + 3 * k + part, piece, meta)
            w = w - piece
    normed[:, feat:] = meta.astype(BF16)

    tok_group = ids[:, 0:1] >> shift
    member = jnp.where(lane == tok_group, 1.0, 0.0)
    earlier = jnp.where(
        lax.broadcasted_iota(jnp.int32, (rows, rows), 1) < lax.broadcasted_iota(jnp.int32, (rows, rows), 0),
        1.0, 0.0,
    ).astype(BF16)
    before = jnp.dot(earlier, member.astype(BF16), preferred_element_type=F32)
    place = jnp.sum(before * member, axis=1, keepdims=True)
    facts = jnp.where(lane == 0, tok_group.astype(F32), jnp.where(lane == 1, place, 0.0))
    pick16 = jnp.where(
        lax.broadcasted_iota(jnp.int32, (16, META), 0) == lax.broadcasted_iota(jnp.int32, (16, META), 1),
        1.0, 0.0,
    ).astype(BF16)
    across = lax.dot_general(pick16, facts.astype(BF16), NT, preferred_element_type=F32)
    group_row, place_row = across[0:1, :], across[1:2, :]
    row_no = lax.broadcasted_iota(jnp.int32, (block, rows), 0).astype(F32)
    tile = 512

    def pack(d):
        hit = (row_no == place_row) & (group_row == flip(group, d).astype(F32))
        pick = jnp.where(hit, 1.0, 0.0).astype(BF16)

        def cols(i, carry):
            c = pl.ds(pl.multiple_of(i * tile, tile), tile)
            x_out[d, :, c] = jnp.dot(pick, normed[:, c], preferred_element_type=F32).astype(BF16)
            return carry

        lax.fori_loop(0, feat // tile, cols, 0)
        x_out[d, :, feat:] = jnp.dot(pick, normed[:, feat:], preferred_element_type=F32).astype(BF16)

    x_copies = {}
    for n, d in enumerate(ORDER):
        pack(d)
        if n == 0:
            pl.semaphore_wait(barrier, GROUPS - 1 + peers - 1)
        x_copies[d] = remote(x_out.at[d], x_in.at[d], xs.at[d], xr.at[d], at(d, 0))
        x_copies[d].start()
    pack(0)

    y_copies, r_copies, h_copies = {}, {}, {}

    def chunk(j):
        return pl.ds(j * capp, capp)

    def dispatch(d):
        src = x_out if d == 0 else x_in
        if d:
            x_copies[d].wait_recv()
        codes = lax.dot_general(pick16, src[d, :, feat:], NT, preferred_element_type=F32)
        slot = (lax.broadcasted_iota(jnp.int32, (spread, block), 0) + 1).astype(F32)
        hit = (slot == codes[0:1, :]) | (slot == codes[1:2, :])
        pick = jnp.where(hit, 1.0, 0.0).astype(BF16)

        def cols(i, carry):
            c = pl.ds(pl.multiple_of(i * tile, tile), tile)
            got = jnp.dot(pick, src[d, :, c], preferred_element_type=F32).astype(BF16)
            e_in[d, :capp, c] = got[:capp]
            y_out[d, capp:, c] = got[capp:]
            return carry

        lax.fori_loop(0, feat // tile, cols, 0)
        for j in range(1, peers):
            copy = remote(y_out.at[d, chunk(j)], e_in.at[d, chunk(j)], ys.at[d, j], yr.at[d, j], at(0, j))
            copy.start()
            y_copies[d, j] = copy

    def compute(d):
        if not r_copies:
            for load in loads:
                load.wait()
        for j in range(1, peers):
            y_copies[d, j].wait_recv()
        half = 256

        def up(i, carry):
            c = pl.ds(pl.multiple_of(i * half, half), half)
            gate = jnp.dot(e_in[d], wg[:, c], preferred_element_type=F32)
            upper = jnp.dot(e_in[d], wu[:, c], preferred_element_type=F32)
            hid[:, c] = (gate / (1.0 + jnp.exp(-gate)) * upper).astype(BF16)
            return carry

        lax.fori_loop(0, ffn // half, up, 0)

        def down(i, carry):
            c = pl.ds(pl.multiple_of(i * tile, tile), tile)
            got = jnp.dot(hid[...], wd[:, c], preferred_element_type=F32).astype(BF16)
            r_in[d, :capp, c] = got[:capp]
            r_out[d, capp:, c] = got[capp:]
            return carry

        lax.fori_loop(0, feat // tile, down, 0)
        for j in range(1, peers):
            copy = remote(r_out.at[d, chunk(j)], r_in.at[d, chunk(j)], rs.at[d, j], rr.at[d, j], at(0, j))
            copy.start()
            r_copies[d, j] = copy

    def combine(d):
        src = x_out if d == 0 else x_in
        for j in range(1, peers):
            r_copies[d, j].wait_recv()
        info = src[d, :, feat:].astype(F32)
        slot = (lax.broadcasted_iota(jnp.int32, (block, spread), 1) + 1).astype(F32)
        picks = [jnp.where(slot == info[:, k:k + 1], 1.0, 0.0).astype(BF16) for k in range(2)]
        weigh = [info[:, 2 + 3 * k:3 + 3 * k] + info[:, 3 + 3 * k:4 + 3 * k] + info[:, 4 + 3 * k:5 + 3 * k] for k in range(2)]

        def cols(i, carry):
            c = pl.ds(pl.multiple_of(i * tile, tile), tile)
            got = r_in[d, :, c]
            mixed = weigh[0] * jnp.dot(picks[0], got, preferred_element_type=F32)
            mixed += weigh[1] * jnp.dot(picks[1], got, preferred_element_type=F32)
            if d == 0:
                h_in[0, :, c] = mixed.astype(BF16)
            else:
                m_out[d, :, c] = mixed.astype(BF16)
            return carry

        lax.fori_loop(0, feat // tile, cols, 0)
        if d:
            h_copies[d] = remote(m_out.at[d], h_in.at[d], hs.at[d], hr.at[d], at(d, 0))
            h_copies[d].start()

    a, b, c = ORDER
    dispatch(0)
    compute(0)
    dispatch(a)
    combine(0)
    compute(a)
    dispatch(b)
    combine(a)
    compute(b)
    dispatch(c)
    combine(b)
    compute(c)
    combine(c)

    local_group = (tok_group ^ group).astype(F32)
    slot = lax.broadcasted_iota(jnp.int32, (rows, block), 1).astype(F32)
    homes = [
        jnp.where((slot == place) & (local_group == float(d)), 1.0, 0.0).astype(BF16)
        for d in range(GROUPS)
    ]
    for d in ORDER:
        h_copies[d].wait_recv()

    def finish(i, carry):
        c = pl.ds(pl.multiple_of(i * tile, tile), tile)
        total = jnp.dot(homes[0], h_in[0, :, c], preferred_element_type=F32)
        for d in range(1, GROUPS):
            total += jnp.dot(homes[d], h_in[d, :, c], preferred_element_type=F32)
        out[:, c] = total.astype(BF16)
        return carry

    lax.fori_loop(0, feat // tile, finish, 0)
    for copies in (x_copies, y_copies, r_copies, h_copies):
        for copy in copies.values():
            copy.wait_send()


def shards(tokens, norm_gain, route_ids, route_slots, route_weights, w_gate, w_up, w_down):
    rows, feat = tokens.shape
    n_devices = lax.axis_size("ep")
    top_count = route_ids.shape[1]
    cap = 3 * top_count * rows // (2 * n_devices)
    capp = -(-cap // 16) * 16
    peers = n_devices // GROUPS
    block = peers * cap // top_count
    spread = peers * capp
    ffn = w_gate.shape[2]
    vmem = pl.BlockSpec(memory_space=pltpu.VMEM)
    anywhere = pl.BlockSpec(memory_space=pl.ANY)
    dma = pltpu.SemaphoreType.DMA
    return pl.pallas_call(
        functools.partial(kernel, peers, cap, capp),
        out_shape=jax.ShapeDtypeStruct((rows, feat), BF16),
        in_specs=[vmem] * 5 + [anywhere] * 3,
        out_specs=vmem,
        scratch_shapes=[
            pltpu.VMEM((rows, feat + META), BF16),
            pltpu.VMEM((GROUPS, block, feat + META), BF16),
            pltpu.VMEM((GROUPS, block, feat + META), BF16),
            pltpu.VMEM((GROUPS, spread, feat), BF16),
            pltpu.VMEM((GROUPS, spread, feat), BF16),
            pltpu.VMEM((spread, ffn), BF16),
            pltpu.VMEM((GROUPS, spread, feat), BF16),
            pltpu.VMEM((GROUPS, spread, feat), BF16),
            pltpu.VMEM((GROUPS, block, feat), BF16),
            pltpu.VMEM((GROUPS, block, feat), BF16),
            pltpu.VMEM((feat, ffn), BF16),
            pltpu.VMEM((feat, ffn), BF16),
            pltpu.VMEM((ffn, feat), BF16),
            dma((3,)),
            dma((GROUPS,)), dma((GROUPS,)),
            dma((GROUPS, peers)), dma((GROUPS, peers)),
            dma((GROUPS, peers)), dma((GROUPS, peers)),
            dma((GROUPS,)), dma((GROUPS,)),
        ],
        compiler_params=pltpu.CompilerParams(
            collective_id=0, has_side_effects=True, vmem_limit_bytes=60 * 1024 * 1024
        ),
    )(
        tokens, norm_gain.reshape(1, feat), route_ids, route_slots, route_weights,
        w_gate.reshape(feat, ffn), w_up.reshape(feat, ffn), w_down.reshape(ffn, feat),
    )


def solution(mesh):
    placed = (
        P(("grp", "ep"), None),
        P(),
        P(("grp", "ep"), None),
        P(("grp", "ep"), None),
        P(("grp", "ep"), None),
        P("ep", None, None),
        P("ep", None, None),
        P("ep", None, None),
    )
    return jax.shard_map(
        shards, mesh=mesh, in_specs=placed, out_specs=P(("grp", "ep"), None), check_vma=False
    )
```

```python
import functools

import jax
import jax.numpy as jnp
from jax import lax
from jax.experimental import pallas as pl
from jax.experimental.pallas import tpu as pltpu
from jax.sharding import PartitionSpec as P

GROUPS = 4
META = 128
CHUNKS = 4
SCHEDULE = (
    "P2", "P0", "D0", "P1", "P3", "H0", "H1", "H2", "H3", "C0", "D2", "D1", "C2", "D3", "M2", "C3", "C1", "M3", "M1", "M0",
)
NT = (((1,), (1,)), ((), ()))
F32 = jnp.float32
BF16 = jnp.bfloat16


def flip(index, bits):
    out, weight = index, 1
    while weight <= bits:
        if bits & weight:
            out = out + weight * (1 - 2 * ((index // weight) % 2))
        weight *= 2
    return out


def where01(hit):
    return jnp.where(hit, 1.0, 0.0).astype(BF16)


def iota(shape, dim):
    return lax.broadcasted_iota(jnp.int32, shape, dim)


def dot(a, b):
    return jnp.dot(a, b, preferred_element_type=F32)


def dot_nt(a, b):
    return lax.dot_general(a, b, NT, preferred_element_type=F32)


def kernel(
    peers, capp,
    tok, gain, ids, slots, wts, wg_hbm, wu_hbm, wd_hbm,
    out,
    normed, meta, n_out, n_in, spreads, picks, homes,
    x_out, x_in, y_out, e_in, hid, r_out, r_in, m_out, h_in, wg, wu, wd,
    w_sem, ns, nr, xs, xr, ys, yr, rs, rr, hs, hr,
):
    rows, feat = tok.shape
    ffn = wg.shape[1]
    block, width = x_out.shape[2:]
    chunks = feat // width
    spread = peers * capp
    me = lax.axis_index("ep")
    group, rank = me // peers, me % peers
    shift = peers.bit_length() - 1
    mesh_id = pl.DeviceIdType.MESH

    def at(d, j):
        return {"ep": flip(group, d) * peers + flip(rank, j)}

    barrier = pltpu.get_barrier_semaphore()
    for d in range(1, GROUPS):
        pl.semaphore_signal(barrier, inc=1, device_id=at(d, 0), device_id_type=mesh_id)
    for j in range(1, peers):
        pl.semaphore_signal(barrier, inc=1, device_id=at(0, j), device_id_type=mesh_id)

    loads = [
        pltpu.make_async_copy(src, dst, w_sem.at[i])
        for i, (src, dst) in enumerate(((wg_hbm, wg), (wu_hbm, wu), (wd_hbm, wd)))
    ]
    for load in loads:
        load.start()

    started = {}

    def send(key, src, dst, sent, got, where):
        copy = pltpu.make_async_remote_copy(
            src_ref=src, dst_ref=dst, send_sem=sent, recv_sem=got,
            device_id=where, device_id_type=mesh_id,
        )
        copy.start()
        started[key] = copy

    step = 32

    def norm_rows(i, carry):
        at_rows = pl.ds(pl.multiple_of(i * step, step), step)
        v = tok[at_rows, :].astype(F32)
        scale = lax.rsqrt(jnp.mean(v * v, axis=-1, keepdims=True) + 1e-06)
        normed[at_rows, :] = (v * scale * gain[...]).astype(BF16)
        return carry

    lax.fori_loop(0, rows // step, norm_rows, 0)

    tok_group = ids[0:1, :] >> shift
    member = where01(iota((16, rows), 0) == tok_group)
    before = dot(member, where01(iota((rows, rows), 0) < iota((rows, rows), 1)))
    place = jnp.sum(before * member.astype(F32), axis=0, keepdims=True)
    kind = iota((META, rows), 0)
    facts = jnp.where(kind == 8, tok_group.astype(F32), jnp.where(kind == 9, place, 0.0))
    for k in range(2):
        code = ((ids[k:k + 1, :] & (peers - 1)) ^ rank) * capp + slots[k:k + 1, :] + 1
        facts = jnp.where(kind == k, code.astype(F32), facts)
        w = wts[k:k + 1, :]
        for part in range(3):
            piece = w.astype(BF16).astype(F32)
            facts = jnp.where(kind == 2 + 3 * k + part, piece, facts)
            w = w - piece
    columns = dot_nt(where01(iota((rows, rows), 0) == iota((rows, rows), 1)), facts.astype(BF16))
    meta[...] = columns.astype(BF16)

    row_no = iota((block, rows), 0).astype(F32)
    tile = min(512, width)

    def tiles(width_of, body):
        def one(i, carry):
            body(pl.multiple_of(i * tile, tile))
            return carry

        lax.fori_loop(0, width_of // tile, one, 0)

    def pack(d):
        chosen = where01((row_no == place) & (tok_group == flip(group, d)))
        n_out[d] = dot(chosen, meta[...]).astype(BF16)
        if d:
            if len(started) == 0:
                pl.semaphore_wait(barrier, GROUPS - 1 + peers - 1)
            send(("n", d), n_out.at[d], n_in.at[d], ns.at[d], nr.at[d], at(d, 0))
        for c in range(chunks):
            def cols(t):
                x_out[d, c, :, pl.ds(t, tile)] = dot(chosen, normed[:, pl.ds(c * width + t, tile)]).astype(BF16)

            tiles(width, cols)
            if d:
                send(("x", d, c), x_out.at[d, c], x_in.at[d, c], xs.at[d, c], xr.at[d, c], at(d, 0))

    def part(j):
        return pl.ds(j * capp, capp)

    far_first = list(range(2, peers)) + [1]

    def dispatch(d):
        src, info = (x_in, n_in) if d else (x_out, n_out)
        if d:
            started["n", d].wait_recv()
        codes = dot_nt(where01(iota((16, META), 0) == iota((16, META), 1)), info[d])
        slot = (iota((spread, block), 0) + 1).astype(F32)
        spreads[d] = where01((slot == codes[0:1, :]) | (slot == codes[1:2, :]))
        for c in range(chunks):
            if d:
                started["x", d, c].wait_recv()

            def cols(t):
                got = dot(spreads[d], src[d, c, :, pl.ds(t, tile)]).astype(BF16)
                e_in[d, c, :capp, pl.ds(t, tile)] = got[:capp]
                y_out[d, c, capp:, pl.ds(t, tile)] = got[capp:]

            tiles(width, cols)
            for j in far_first:
                send(("y", d, c, j), y_out.at[d, c, part(j)], e_in.at[d, c, part(j)],
                     ys.at[d, c, j], yr.at[d, c, j], at(0, j))
        slot = (iota((block, spread), 1) + 1).astype(F32)
        about = info[d].astype(F32)
        for k in range(2):
            picks[d, k] = where01(slot == about[:, k:k + 1])

    def compute(d):
        if loads:
            for load in loads:
                load.wait()
            loads.clear()
        half = 256
        for c in range(chunks):
            for j in range(1, peers):
                started["y", d, c, j].wait_recv()

        def up(i, carry):
            f = pl.ds(pl.multiple_of(i * half, half), half)
            gate = sum(dot(e_in[d, c], wg[c * width:(c + 1) * width, f]) for c in range(chunks))
            upper = sum(dot(e_in[d, c], wu[c * width:(c + 1) * width, f]) for c in range(chunks))
            hid[:, f] = (gate / (1.0 + jnp.exp(-gate)) * upper).astype(BF16)
            return carry

        lax.fori_loop(0, ffn // half, up, 0)
        for c in range(chunks):
            def down(t):
                got = dot(hid[...], wd[:, pl.ds(c * width + t, tile)]).astype(BF16)
                r_in[d, c, :capp, pl.ds(t, tile)] = got[:capp]
                r_out[d, c, capp:, pl.ds(t, tile)] = got[capp:]

            tiles(width, down)
            for j in far_first:
                send(("r", d, c, j), r_out.at[d, c, part(j)], r_in.at[d, c, part(j)],
                     rs.at[d, c, j], rr.at[d, c, j], at(0, j))

    def combine(d):
        info = (n_in if d else n_out)[d].astype(F32)
        weigh = [info[:, b:b + 1] + info[:, b + 1:b + 2] + info[:, b + 2:b + 3] for b in (2, 5)]
        dst = m_out if d else h_in
        for c in range(chunks):
            for j in range(1, peers):
                started["r", d, c, j].wait_recv()

            def cols(t):
                got = r_in[d, c, :, pl.ds(t, tile)]
                mixed = weigh[0] * dot(picks[d, 0], got) + weigh[1] * dot(picks[d, 1], got)
                dst[d, c, :, pl.ds(t, tile)] = mixed.astype(BF16)

            tiles(width, cols)
            if d:
                send(("h", d, c), m_out.at[d, c], h_in.at[d, c], hs.at[d, c], hr.at[d, c], at(d, 0))

    def aim(d):
        slot = iota((rows, block), 1).astype(F32)
        homes[d] = where01((slot == columns[:, 9:10]) & (columns[:, 8:9] == flip(group, d).astype(F32)))

    stages = {"P": pack, "D": dispatch, "C": compute, "M": combine, "H": aim}
    for item in SCHEDULE:
        stages[item[0]](int(item[1]))

    for c in range(chunks):
        for d in range(1, GROUPS):
            started["h", d, c].wait_recv()

        def finish(t):
            total = dot(homes[0], h_in[0, c, :, pl.ds(t, tile)])
            for d in range(1, GROUPS):
                total += dot(homes[d], h_in[d, c, :, pl.ds(t, tile)])
            out[:, pl.ds(c * width + t, tile)] = total.astype(BF16)

        tiles(width, finish)
    for copy in started.values():
        copy.wait_send()


def shards(tokens, norm_gain, route_ids, route_slots, route_weights, w_gate, w_up, w_down):
    rows, feat = tokens.shape
    n_devices = lax.axis_size("ep")
    top_count = route_ids.shape[1]
    cap = 3 * top_count * rows // (2 * n_devices)
    capp = -(-cap // 16) * 16
    peers = n_devices // GROUPS
    block = peers * cap // top_count
    spread = peers * capp
    ffn = w_gate.shape[2]
    width = feat // CHUNKS
    vmem = pl.BlockSpec(memory_space=pltpu.VMEM)
    anywhere = pl.BlockSpec(memory_space=pl.ANY)
    dma = pltpu.SemaphoreType.DMA

    def buf(*shape):
        return pltpu.VMEM(shape, BF16)

    return pl.pallas_call(
        functools.partial(kernel, peers, capp),
        out_shape=jax.ShapeDtypeStruct((rows, feat), BF16),
        in_specs=[vmem] * 5 + [anywhere] * 3,
        out_specs=vmem,
        scratch_shapes=[
            buf(rows, feat), buf(rows, META),
            buf(GROUPS, block, META), buf(GROUPS, block, META),
            buf(GROUPS, spread, block), buf(GROUPS, 2, block, spread), buf(GROUPS, rows, block),
            buf(GROUPS, CHUNKS, block, width), buf(GROUPS, CHUNKS, block, width),
            buf(GROUPS, CHUNKS, spread, width), buf(GROUPS, CHUNKS, spread, width),
            buf(spread, ffn),
            buf(GROUPS, CHUNKS, spread, width), buf(GROUPS, CHUNKS, spread, width),
            buf(GROUPS, CHUNKS, block, width), buf(GROUPS, CHUNKS, block, width),
            buf(feat, ffn), buf(feat, ffn), buf(ffn, feat),
            dma((3,)),
            dma((GROUPS,)), dma((GROUPS,)),
            dma((GROUPS, CHUNKS)), dma((GROUPS, CHUNKS)),
            dma((GROUPS, CHUNKS, peers)), dma((GROUPS, CHUNKS, peers)),
            dma((GROUPS, CHUNKS, peers)), dma((GROUPS, CHUNKS, peers)),
            dma((GROUPS, CHUNKS)), dma((GROUPS, CHUNKS)),
        ],
        compiler_params=pltpu.CompilerParams(
            collective_id=0, has_side_effects=True, vmem_limit_bytes=60 * 1024 * 1024
        ),
    )(
        tokens, norm_gain.reshape(1, feat), route_ids.T, route_slots.T, route_weights.T,
        w_gate.reshape(feat, ffn), w_up.reshape(feat, ffn), w_down.reshape(ffn, feat),
    )


def solution(mesh):
    placed = (
        P(("grp", "ep"), None),
        P(),
        P(("grp", "ep"), None),
        P(("grp", "ep"), None),
        P(("grp", "ep"), None),
        P("ep", None, None),
        P("ep", None, None),
        P("ep", None, None),
    )
    return jax.shard_map(
        shards, mesh=mesh, in_specs=placed, out_specs=P(("grp", "ep"), None), check_vma=False
    )
```
